32 devices in a mesh: ep: 32 (over z, y, x, core).
Axes of the slice: x: 2, y: 2, z: 4, core: 2. Of those that a mesh axis runs over, the one named last changes fastest.
Arguments:
- tokens: bfloat16 [4096, 2048], P('ep'), may hold values from -6 to 6
- norm_gain: float32 [2048], replicated, may hold values from 0.1 to 1.9
- route_ids: int32 [4096, 2], P('ep'), may hold values from 0 to 31, all different within a row; in each aligned block of 128 rows (0 to 127, 128 to 255, ...) at most 8 rows name the same one
- route_weight: float32 [4096, 2], P('ep'), may hold values from 0.25 to 1
- expert_gate: bfloat16 [32, 2048, 1024], P('ep'), may hold values from -0.125 to 0.125
- expert_up: bfloat16 [32, 2048, 1024], P('ep'), may hold values from -0.125 to 0.125
- expert_down: bfloat16 [32, 1024, 2048], P('ep'), may hold values from -0.1875 to 0.1875
- dense_up: bfloat16 [2048, 512], P('ep'), may hold values from -0.125 to 0.125
- dense_down: bfloat16 [512, 2048], P(None, 'ep'), may hold values from -0.25 to 0.25
- branch_gate: float32 [2048], replicated, may hold values from -1.5 to 1.5
Outputs:
- mixed: bfloat16 [4096, 2048], P('ep')
The draws below stay inside these ranges and needn't reach their ends.
Inputs may be any that keep to these rules, and one draw needn't show every extreme that they name: `route_ids`: each token names 2 different experts; among the 128 tokens of one device (aligned blocks of rows) no expert is named more than 8 times, and in every draw some expert is named exactly 8 times by some device's tokens; every expert is named by some token.
All inputs are finite; a program needn't handle non-finite values.
Results may differ from the reference program's by a relative error of at most 0.01.
Values may be sent and summed in bfloat16 or wider, within the bound.
A program may use at most 128 MiB of HBM per device.

```python
import math
import jax
import jax.numpy as jnp
import numpy as np
from jax import lax

D = 2048
FF = 1024
DH = 512
TOP = 2
CAP = 8
TOK_DEV = 128
TOKENS = 4096
EXPERTS = 32
N_EP = 32


def steps_of(key, extent, split, smallest, top_value):
    def one(dim, blocks):
        heights = jax.random.uniform(jax.random.fold_in(jax.random.fold_in(key, 6), dim), (blocks,), jnp.float32, smallest / len(split), top_value / len(split))
        return jnp.repeat(jnp.exp(heights), extent[dim] // blocks).reshape((-1,) + (1,) * (len(extent) - dim - 1))

    level = one(*split[0])
    for cut in split[1:]:
        level = level * one(*cut)
    return level


def shared_out(own_key, own, number, rows, count, top, limit, lean):
    ranking = jax.random.permutation(own_key, count)
    crowded, common = load_shares(count, rows * top, limit, lean, True), load_shares(count, rows * top, limit, lean, False)
    places = jnp.arange(count)

    def named(sizes, rotation):
        used = int((sizes > 0).sum())
        fixed = max(1, used // 4)
        moved = fixed + (places - fixed + rotation * (used - fixed)) % max(1, count - fixed)
        return jnp.zeros((count,), jnp.int32).at[ranking[jnp.where(places < fixed, places, moved)]].set(jnp.asarray(sizes, jnp.int32))

    sizes = jnp.where(number % 4 == 0, named(crowded, number // 4), named(common, number - number // 4 - 1))
    mixed = jax.random.permutation(jax.random.fold_in(own, 3), count)
    source_of, taker = mixed[0:count // 2 * 2:2], mixed[1:count // 2 * 2:2]
    slack = jnp.minimum(sizes[source_of] - 1, limit - sizes[taker]) // 2
    slack = jnp.where((source_of == ranking[0]) | (taker == ranking[0]) | (sizes[taker] == 0), 0, jnp.maximum(slack, 0))
    moved = jax.random.randint(jax.random.fold_in(own, 4), (count // 2,), 0, 1 << 20) % (slack + 1)
    sizes = sizes.at[source_of].add(-moved).at[taker].add(moved)
    labels = jnp.searchsorted(jnp.cumsum(sizes), jnp.arange(rows * top), side="right").astype(jnp.int32)
    grid = labels.reshape(top, rows).T
    grid = grid[jax.random.permutation(jax.random.fold_in(own, 1), rows)]
    rotation = jax.random.randint(jax.random.fold_in(own, 2), (rows, 1), 0, top)
    return jnp.take_along_axis(grid, (jnp.arange(top)[None, :] + rotation) % top, axis=1)


def load_shares(count, total, bound, slope, full):
    weights = [(1 << 20) // math.isqrt(rank ** slope) + 1 for rank in range(1, count + 1)]
    largest = bound if full else min(bound, max(-(-total // count), total * weights[0] // sum(weights)))
    least = 1 if total - largest >= count - 1 else 0
    counts, spare = [largest] + [least] * (count - 1), total - largest - least * (count - 1)
    while spare > 0:
        candidates = [i for i in range(1, count) if counts[i] < largest] or [i for i in range(1, count) if counts[i] < bound]
        whole, budget = sum([weights[i] for i in candidates]), spare
        for i in candidates:
            addition = min(bound - counts[i], max(1, budget * weights[i] // whole), spare)
            counts[i] = counts[i] + addition
            spare = spare - addition
    return np.array(counts)


def scatter_about(rng, extent, deviation, reach, split=(), kind=jnp.bfloat16):
    gain = steps_of(rng, extent, split, -0.22, 0.18) if split else 1.0
    values = jax.random.normal(rng, extent, jnp.float32) * deviation * gain
    return jnp.minimum(jnp.maximum(values, -reach), reach).astype(kind)


def setup_inputs(seed: int = 0) -> dict:
    streams_of = jax.random.split(jax.random.key(seed), 11)
    tokens = scatter_about(streams_of[0], (TOKENS, D), 1.0, 6.0, ((0, 32),))
    norm_gain = jnp.clip(1.0 + 0.18 * jax.random.normal(streams_of[1], (D,), jnp.float32), 0.1, 1.9)
    route_ids_keys = jax.random.split(jax.random.fold_in(streams_of[2], 1), TOKENS // TOK_DEV)
    route_ids_turns = jax.random.permutation(jax.random.fold_in(streams_of[2], 3), TOKENS // TOK_DEV)
    route_ids = jax.vmap(lambda own, number: shared_out(jax.random.fold_in(streams_of[2], 2), own, number, TOK_DEV, EXPERTS, TOP, CAP, 2))(route_ids_keys, route_ids_turns).reshape((TOKENS, TOP))
    route_weight = jnp.clip(0.25 + 0.75 * jax.random.uniform(streams_of[3], (TOKENS, TOP), jnp.float32) ** steps_of(streams_of[3], (TOKENS, TOP), ((0, 32),), -0.2, 0.2), 0.25, 1.0)
    expert_gate = scatter_about(streams_of[4], (EXPERTS, D, FF), D ** -0.5, 0.125, ((0, 32),))
    expert_up = scatter_about(streams_of[5], (EXPERTS, D, FF), D ** -0.5, 0.125, ((0, 32),))
    expert_down = scatter_about(streams_of[6], (EXPERTS, FF, D), FF ** -0.5, 0.1875, ((0, 32),))
    dense_up = scatter_about(streams_of[7], (D, DH), D ** -0.5, 0.125, ((0, 32),))
    dense_down = scatter_about(streams_of[8], (DH, D), DH ** -0.5, 0.25, ((1, 32),))
    branch_gate = jnp.clip(jax.random.uniform(streams_of[9], (D,), jnp.float32, -1.5, 1.5), -1.5, 1.5)
    return dict(tokens=tokens, norm_gain=norm_gain, route_ids=route_ids, route_weight=route_weight, expert_gate=expert_gate, expert_up=expert_up, expert_down=expert_down, dense_up=dense_up, dense_down=dense_down, branch_gate=branch_gate)


def reference(tokens, norm_gain, route_ids, route_weight, expert_gate, expert_up, expert_down, dense_up, dense_down, branch_gate):
    wide_tokens = tokens.astype(jnp.float32)
    scale = lax.rsqrt(lax.optimization_barrier(jnp.mean(wide_tokens * wide_tokens, axis=-1, keepdims=True)) + 1e-06)
    normed = (wide_tokens * scale * norm_gain).astype(jnp.bfloat16)
    flat_ids = route_ids.reshape(-1).astype(jnp.int32)
    entries = TOKENS * TOP
    onehot = (flat_ids[:, None] == jnp.arange(EXPERTS, dtype=jnp.int32)[None, :]).astype(jnp.int32)
    blocked = onehot.reshape(N_EP, TOK_DEV * TOP, EXPERTS)
    earlier = (jnp.cumsum(blocked, axis=1) - blocked).reshape(entries, EXPERTS)
    slot_index = lax.optimization_barrier(jnp.sum(earlier * onehot, axis=-1)).astype(jnp.int32)
    source = (jnp.arange(entries, dtype=jnp.int32) // (TOK_DEV * TOP)).astype(jnp.int32)
    position = (source * CAP + slot_index).astype(jnp.int32)
    token_index = (jnp.arange(entries, dtype=jnp.int32) // TOP).astype(jnp.int32)
    table = jnp.full((EXPERTS, N_EP * CAP), TOKENS, jnp.int32).at[flat_ids, position].set(token_index)
    weight_table = jnp.zeros((EXPERTS, N_EP * CAP), jnp.float32).at[flat_ids, position].set(route_weight.reshape(-1).astype(jnp.float32))
    padded = jnp.concatenate([normed, jnp.zeros((1, D), jnp.bfloat16)], axis=0)

    def expert_step(summed, inputs):
        row_table, row_weight, w_gate, w_up, w_down = inputs
        row_block = jnp.take(padded, row_table, axis=0)
        gate_part = jnp.dot(row_block, w_gate, preferred_element_type=jnp.float32)
        up_part = jnp.dot(row_block, w_up, preferred_element_type=jnp.float32)
        hidden = (jax.nn.silu(gate_part) * up_part).astype(jnp.bfloat16)
        result = jnp.dot(hidden, w_down, preferred_element_type=jnp.float32).astype(jnp.bfloat16)
        weighted = result.astype(jnp.float32) * row_weight[:, None]
        return (summed.at[row_table].add(weighted), None)
    summed, _ = lax.scan(expert_step, jnp.zeros((TOKENS + 1, D), jnp.float32), (table, weight_table, expert_gate, expert_up, expert_down))
    combined = summed[:TOKENS]
    dense_pre = jnp.dot(normed, dense_up, preferred_element_type=jnp.float32)
    dense_hidden = jax.nn.silu(dense_pre).astype(jnp.bfloat16)
    dense_out = jnp.dot(dense_hidden, dense_down, preferred_element_type=jnp.float32)
    return (combined + jnp.tanh(branch_gate) * dense_out).astype(jnp.bfloat16)
```

```python
import functools
import math

import jax
import jax.numpy as jnp
from jax import lax
from jax.experimental import pallas as pl
from jax.experimental.pallas import tpu as pltpu
from jax.sharding import PartitionSpec as P

CAP = 8
F32 = jnp.float32
BF16 = jnp.bfloat16


def xor(a, b, size):
    out, bit = 0, 1
    while bit < size:
        out = out + ((a // bit) % 2 + (b // bit) % 2) % 2 * bit
        bit *= 2
    return out


def kernel(
    dims,
    tokens, gain, ids, weight, w_gate, w_up, w_down, d_up, d_down, branch,
    out,
    normed, send, recv, result, back, v_gate, v_up, v_down, wide,
    local_sem, out_send, out_recv, ret_send, ret_recv,
    z_send, z_recv, y_send, y_recv, x_send, x_recv, c_send, c_recv,
):
    n_z, n_y, n_x, n_c = dims
    plane = n_y * n_x * n_c
    n = n_z * plane
    me = lax.axis_index("ep")
    my_z = me // plane
    my_in = me % plane
    my_c = me % n_c
    my_x = me // n_c % n_x
    my_y = me // (n_c * n_x) % n_y
    rows = tokens.shape[0]
    width = tokens.shape[1]
    experts = n
    slots = experts * CAP

    def dev(z, y, x, c):
        return ((z * n_y + y) * n_x + x) * n_c + c

    barrier = pltpu.get_barrier_semaphore()

    def greet(i, carry):
        pl.semaphore_signal(barrier, inc=1, device_id=((me + i) % n,), device_id_type=pl.DeviceIdType.MESH)
        return carry

    lax.fori_loop(1, n, greet, 0)

    own_up = pltpu.make_async_copy(d_up, wide.at[0, my_z, my_y, my_x, my_c], local_sem.at[0])
    own_down = pltpu.make_async_copy(d_down, wide.at[1, my_z, my_y, my_x, my_c], local_sem.at[1])
    own_up.start()
    own_down.start()
    loads = [
        pltpu.make_async_copy(w_gate.at[0], v_gate, local_sem.at[2]),
        pltpu.make_async_copy(w_up.at[0], v_up, local_sem.at[3]),
        pltpu.make_async_copy(w_down.at[0], v_down, local_sem.at[4]),
    ]
    for load in loads:
        load.start()

    x = tokens[...].astype(F32)
    scale = lax.rsqrt(jnp.mean(x * x, axis=-1, keepdims=True) + 1e-06)
    normed[...] = (x * scale * gain[...]).astype(BF16)

    id0, id1 = ids[0:1, :], ids[1:2, :]
    e_iota = lax.broadcasted_iota(jnp.int32, (experts, rows), 0)
    hot0 = (id0 == e_iota).astype(F32)
    hot1 = (id1 == e_iota).astype(F32)
    before = lax.broadcasted_iota(jnp.int32, (rows, rows), 0) < lax.broadcasted_iota(jnp.int32, (rows, rows), 1)
    count = jnp.dot((hot0 + hot1).astype(BF16), before.astype(F32).astype(BF16), preferred_element_type=F32)
    pos0 = id0 * CAP + jnp.sum(hot0 * count, axis=0, keepdims=True).astype(jnp.int32)
    pos1 = id1 * CAP + jnp.sum(hot1 * count, axis=0, keepdims=True).astype(jnp.int32)
    p_iota = lax.broadcasted_iota(jnp.int32, (slots, rows), 0)
    table0 = (pos0 == p_iota).astype(F32)
    table1 = (pos1 == p_iota).astype(F32)
    place = (table0 + table1).astype(BF16)
    packed = jnp.dot(place, normed[...], preferred_element_type=F32)
    send[...] = packed.reshape(n, CAP, width).astype(BF16)

    own_up.wait()
    own_down.wait()
    pl.semaphore_wait(barrier, n - 1)

    def remote(src, dst, s, r, target):
        return pltpu.make_async_remote_copy(
            src_ref=src, dst_ref=dst, send_sem=s, recv_sem=r,
            device_id=(target,), device_id_type=pl.DeviceIdType.MESH,
        )

    def z_copy(d, origin):
        part = wide.at[:, origin, my_y, my_x, my_c]
        return remote(part, part, z_send.at[d], z_recv.at[d], dev((my_z + d) % n_z, my_y, my_x, my_c))

    def y_copy(d, origin):
        part = wide.at[:, :, origin, my_x, my_c]
        return remote(part, part, y_send.at[d], y_recv.at[d], dev(my_z, (my_y + d) % n_y, my_x, my_c))

    def x_copy(d, origin):
        part = wide.at[:, :, :, origin, my_c]
        return remote(part, part, x_send.at[d], x_recv.at[d], dev(my_z, my_y, (my_x + d) % n_x, my_c))

    def c_copy(d, origin):
        part = wide.at[:, :, :, :, origin]
        return remote(part, part, c_send.at[d], c_recv.at[d], dev(my_z, my_y, my_x, (my_c + d) % n_c))

    stages = [(z_copy, n_z, my_z), (y_copy, n_y, my_y), (x_copy, n_x, my_x), (c_copy, n_c, my_c)]

    def begin(stage):
        copy, size, at = stages[stage]
        for d in range(1, size):
            copy(d, at).start()

    def arrive(stage):
        copy, size, at = stages[stage]
        for d in range(1, size):
            copy(d, (at + size - d) % size).wait_recv()

    def leave(stage):
        copy, size, at = stages[stage]
        for d in range(1, size):
            copy(d, at).wait_send()

    begin(0)

    def partner(step):
        z = xor(my_z, (step // plane + n_z // 2) % n_z, n_z)
        return z * plane + xor(my_in, step % plane, plane)

    own_step = (n_z - n_z // 2) * plane

    def over_others(first, last, body):
        def guarded(step, carry):
            body(partner(step))
            return carry

        if first <= own_step < last:
            lax.fori_loop(first, own_step, guarded, 0)
            lax.fori_loop(own_step + 1, last, guarded, 0)
        else:
            lax.fori_loop(first, last, guarded, 0)

    def dispatch(target, origin):
        return remote(send.at[target], recv.at[origin], out_send.at[target], out_recv.at[origin], target)

    def giveback(target, origin):
        return remote(result.at[target], back.at[origin], ret_send.at[target], ret_recv.at[origin], target)

    over_others(0, n, lambda t: dispatch(t, me).start())
    recv[me] = send[me]

    for load in loads:
        load.wait()

    def experts_on(phase):
        z = xor(my_z, (phase + n_z // 2) % n_z, n_z)
        block = pl.ds(z * plane, plane)
        x_in = recv[block].reshape(plane * CAP, width)
        gate_part = jnp.dot(x_in, v_gate[...], preferred_element_type=F32)
        up_part = jnp.dot(x_in, v_up[...], preferred_element_type=F32)
        hidden = (gate_part / (1.0 + jnp.exp(-gate_part)) * up_part).astype(BF16)
        res = jnp.dot(hidden, v_down[...], preferred_element_type=F32)
        result[block] = res.reshape(plane, CAP, width).astype(BF16)

    arrive(0)
    begin(1)

    def do_phase(phase):
        lo, hi = phase * plane, (phase + 1) * plane
        over_others(lo, hi, lambda t: dispatch(me, t).wait_recv())
        experts_on(phase)
        over_others(lo, hi, lambda t: giveback(t, me).start())

    for phase in range(n_z):
        do_phase(phase)
        if phase < 3:
            arrive(phase + 1)
            if phase < 2:
                begin(phase + 2)

    back[me] = result[me]

    dense_pre = jnp.dot(normed[...], wide[0].reshape(width, -1), preferred_element_type=F32)
    dense_hidden = (dense_pre / (1.0 + jnp.exp(-dense_pre))).astype(BF16)
    dense_out = lax.dot_general(
        dense_hidden, wide[1].reshape(width, -1), (((1,), (1,)), ((), ())), preferred_element_type=F32
    )
    dense_out = jnp.tanh(branch[...]) * dense_out

    share = table0 * weight[0:1, :] + table1 * weight[1:2, :]
    high = share.astype(BF16)
    low = (share - high.astype(F32)).astype(BF16)

    over_others(0, n, lambda t: giveback(me, t).wait_recv())
    rows_back = back[...].reshape(slots, width)
    across = (((0,), (0,)), ((), ()))
    combined = lax.dot_general(high, rows_back, across, preferred_element_type=F32)
    combined = combined + lax.dot_general(low, rows_back, across, preferred_element_type=F32)
    out[...] = (combined + dense_out).astype(BF16)

    over_others(0, n, lambda t: dispatch(t, me).wait_send())
    over_others(0, n, lambda t: giveback(t, me).wait_send())
    for stage in range(4):
        leave(stage)


def on_device(tokens, norm_gain, route_ids, route_weight, expert_gate, expert_up, expert_down, dense_up, dense_down, branch_gate):
    n = lax.axis_size("ep")
    assert expert_gate.shape[0] == 1
    rows, width = tokens.shape
    ff = expert_gate.shape[2]
    d_rows, dh = dense_up.shape
    n_z = 4
    side = math.isqrt(n // n_z // 2)
    dims = (n_z, side, side, 2)
    assert math.prod(dims) == n
    vmem = pl.BlockSpec(memory_space=pltpu.VMEM)
    hbm = pl.BlockSpec(memory_space=pl.ANY)
    dma = pltpu.SemaphoreType.DMA
    return pl.pallas_call(
        functools.partial(kernel, dims),
        out_shape=jax.ShapeDtypeStruct((rows, width), BF16),
        in_specs=[vmem, vmem, vmem, vmem, hbm, hbm, hbm, hbm, hbm, vmem],
        out_specs=vmem,
        scratch_shapes=[
            pltpu.VMEM((rows, width), BF16),
            pltpu.VMEM((n, CAP, width), BF16),
            pltpu.VMEM((n, CAP, width), BF16),
            pltpu.VMEM((n, CAP, width), BF16),
            pltpu.VMEM((n, CAP, width), BF16),
            pltpu.VMEM((width, ff), BF16),
            pltpu.VMEM((width, ff), BF16),
            pltpu.VMEM((ff, width), BF16),
            pltpu.VMEM((2,) + dims + (d_rows, dh), BF16),
            dma((5,)), dma((n,)), dma((n,)), dma((n,)), dma((n,)),
            dma((n_z,)), dma((n_z,)), dma((side,)), dma((side,)),
            dma((side,)), dma((side,)), dma((2,)), dma((2,)),
        ],
        compiler_params=pltpu.CompilerParams(
            collective_id=0, has_side_effects=True, vmem_limit_bytes=60 * 1024 * 1024
        ),
    )(
        tokens, norm_gain.reshape(1, -1), route_ids.T, route_weight.T,
        expert_gate, expert_up, expert_down, dense_up, dense_down.T, branch_gate.reshape(1, -1),
    )


def solution(mesh):
    placed = (
        P("ep", None), P(), P("ep", None), P("ep", None),
        P("ep", None, None), P("ep", None, None), P("ep", None, None),
        P("ep", None), P(None, "ep"), P(),
    )
    return jax.shard_map(
        on_device, mesh=mesh, in_specs=placed, out_specs=P("ep", None), check_vma=False
    )
```

```python
import functools
import math

import jax
import jax.numpy as jnp
from jax import lax
from jax.experimental import pallas as pl
from jax.experimental.pallas import tpu as pltpu
from jax.sharding import PartitionSpec as P

CAP = 8
F32 = jnp.float32
BF16 = jnp.bfloat16


def xor(a, b, size):
    out, bit = 0, 1
    while bit < size:
        out = out + ((a // bit) % 2 + (b // bit) % 2) % 2 * bit
        bit *= 2
    return out


def kernel(
    dims,
    tokens, gain, ids, weight, w_gate, w_up, w_down, d_up, d_down, branch,
    out,
    normed, send, recv, result, back, v_gate, v_up, v_down, wide,
    local_sem, out_send, out_recv, ret_send, ret_recv,
    w_send, w_recv,
):
    n_z, n_y, n_x, n_c = dims
    plane = n_y * n_x * n_c
    n = n_z * plane
    me = lax.axis_index("ep")
    my_z = me // plane
    my_in = me % plane
    my_c = me % n_c
    my_x = me // n_c % n_x
    my_y = me // (n_c * n_x) % n_y
    rows = tokens.shape[0]
    width = tokens.shape[1]
    experts = n
    slots = experts * CAP

    def dev(z, y, x, c):
        return ((z * n_y + y) * n_x + x) * n_c + c

    barrier = pltpu.get_barrier_semaphore()

    def greet(i, carry):
        pl.semaphore_signal(barrier, inc=1, device_id=((me + i) % n,), device_id_type=pl.DeviceIdType.MESH)
        return carry

    lax.fori_loop(1, n, greet, 0)

    own_up = pltpu.make_async_copy(d_up, wide.at[0, my_z, my_y, my_x, my_c], local_sem.at[0])
    own_down = pltpu.make_async_copy(d_down, wide.at[1, my_z, my_y, my_x, my_c], local_sem.at[1])
    own_up.start()
    own_down.start()
    loads = [
        pltpu.make_async_copy(w_gate.at[0], v_gate, local_sem.at[2]),
        pltpu.make_async_copy(w_up.at[0], v_up, local_sem.at[3]),
        pltpu.make_async_copy(w_down.at[0], v_down, local_sem.at[4]),
    ]
    for load in loads:
        load.start()

    x = tokens[...].astype(F32)
    scale = lax.rsqrt(jnp.mean(x * x, axis=-1, keepdims=True) + 1e-06)
    normed[...] = (x * scale * gain[...]).astype(BF16)

    id0, id1 = ids[0:1, :], ids[1:2, :]
    e_iota = lax.broadcasted_iota(jnp.int32, (experts, rows), 0)
    hot0 = (id0 == e_iota).astype(F32)
    hot1 = (id1 == e_iota).astype(F32)
    before = lax.broadcasted_iota(jnp.int32, (rows, rows), 0) < lax.broadcasted_iota(jnp.int32, (rows, rows), 1)
    count = jnp.dot((hot0 + hot1).astype(BF16), before.astype(F32).astype(BF16), preferred_element_type=F32)
    pos0 = id0 * CAP + jnp.sum(hot0 * count, axis=0, keepdims=True).astype(jnp.int32)
    pos1 = id1 * CAP + jnp.sum(hot1 * count, axis=0, keepdims=True).astype(jnp.int32)
    p_iota = lax.broadcasted_iota(jnp.int32, (slots, rows), 0)
    table0 = (pos0 == p_iota).astype(F32)
    table1 = (pos1 == p_iota).astype(F32)
    place = (table0 + table1).astype(BF16)
    packed = jnp.dot(place, normed[...], preferred_element_type=F32)
    send[...] = packed.reshape(n, CAP, width).astype(BF16)

    own_up.wait()
    own_down.wait()
    pl.semaphore_wait(barrier, n - 1)

    def remote(src, dst, s, r, target):
        return pltpu.make_async_remote_copy(
            src_ref=src, dst_ref=dst, send_sem=s, recv_sem=r,
            device_id=(target,), device_id_type=pl.DeviceIdType.MESH,
        )

    at = (my_z, my_y, my_x, my_c)
    orders = ((0, 1, 2, 3), (0, 2, 1, 3))

    def block_copy(half, stage, d, incoming):
        order = orders[half]
        axis = order[stage]
        origin = (at[axis] + dims[axis] - d) % dims[axis] if incoming else at[axis]
        where = [at[i] for i in range(4)]
        for held in order[:stage]:
            where[held] = slice(None)
        where[axis] = origin
        part = wide.at[(half,) + tuple(where)]
        target = [at[i] for i in range(4)]
        target[axis] = (at[axis] + d) % dims[axis]
        return remote(part, part, w_send.at[half, stage, d], w_recv.at[half, stage, d], dev(*target))

    def each(stage, act, incoming=False):
        for half in range(2):
            for d in range(1, dims[orders[half][stage]]):
                act(block_copy(half, stage, d, incoming))

    def begin(stage):
        each(stage, lambda copy: copy.start())

    def arrive(stage):
        each(stage, lambda copy: copy.wait_recv(), True)

    def leave(stage):
        each(stage, lambda copy: copy.wait_send())

    begin(0)

    def partner(step):
        z = xor(my_z, (step // plane + n_z // 2) % n_z, n_z)
        return z * plane + xor(my_in, step % plane, plane)

    own_step = (n_z - n_z // 2) * plane

    def over_others(first, last, body):
        def guarded(step, carry):
            body(partner(step))
            return carry

        if first <= own_step < last:
            lax.fori_loop(first, own_step, guarded, 0)
            lax.fori_loop(own_step + 1, last, guarded, 0)
        else:
            lax.fori_loop(first, last, guarded, 0)

    def dispatch(target, origin):
        return remote(send.at[target], recv.at[origin], out_send.at[target], out_recv.at[origin], target)

    def giveback(target, origin):
        return remote(result.at[target], back.at[origin], ret_send.at[target], ret_recv.at[origin], target)

    over_others(0, n, lambda t: dispatch(t, me).start())
    recv[me] = send[me]

    for load in loads:
        load.wait()

    def experts_on(phase):
        z = xor(my_z, (phase + n_z // 2) % n_z, n_z)
        block = pl.ds(z * plane, plane)
        x_in = recv[block].reshape(plane * CAP, width)
        gate_part = jnp.dot(x_in, v_gate[...], preferred_element_type=F32)
        up_part = jnp.dot(x_in, v_up[...], preferred_element_type=F32)
        hidden = (gate_part / (1.0 + jnp.exp(-gate_part)) * up_part).astype(BF16)
        res = jnp.dot(hidden, v_down[...], preferred_element_type=F32)
        result[block] = res.reshape(plane, CAP, width).astype(BF16)

    arrive(0)
    begin(1)

    def do_phase(phase):
        lo, hi = phase * plane, (phase + 1) * plane
        over_others(lo, hi, lambda t: dispatch(me, t).wait_recv())
        experts_on(phase)
        over_others(lo, hi, lambda t: giveback(t, me).start())

    for phase in range(n_z):
        do_phase(phase)
        if phase == 0:
            arrive(1)
            begin(2)
        if phase == 2:
            arrive(2)
            begin(3)
        if phase == 3:
            arrive(3)

    back[me] = result[me]

    dense_pre = jnp.dot(normed[...], wide[0].reshape(width, -1), preferred_element_type=F32)
    dense_hidden = (dense_pre / (1.0 + jnp.exp(-dense_pre))).astype(BF16)
    dense_out = lax.dot_general(
        dense_hidden, wide[1].reshape(width, -1), (((1,), (1,)), ((), ())), preferred_element_type=F32
    )
    dense_out = jnp.tanh(branch[...]) * dense_out

    share = table0 * weight[0:1, :] + table1 * weight[1:2, :]
    high = share.astype(BF16)
    low = (share - high.astype(F32)).astype(BF16)

    over_others(0, n, lambda t: giveback(me, t).wait_recv())
    rows_back = back[...].reshape(slots, width)
    across = (((0,), (0,)), ((), ()))
    combined = lax.dot_general(high, rows_back, across, preferred_element_type=F32)
    combined = combined + lax.dot_general(low, rows_back, across, preferred_element_type=F32)
    out[...] = (combined + dense_out).astype(BF16)

    over_others(0, n, lambda t: dispatch(t, me).wait_send())
    over_others(0, n, lambda t: giveback(t, me).wait_send())
    for stage in range(4):
        leave(stage)


def on_device(tokens, norm_gain, route_ids, route_weight, expert_gate, expert_up, expert_down, dense_up, dense_down, branch_gate):
    n = lax.axis_size("ep")
    assert expert_gate.shape[0] == 1
    rows, width = tokens.shape
    ff = expert_gate.shape[2]
    d_rows, dh = dense_up.shape
    n_z = 4
    side = math.isqrt(n // n_z // 2)
    dims = (n_z, side, side, 2)
    assert math.prod(dims) == n
    vmem = pl.BlockSpec(memory_space=pltpu.VMEM)
    hbm = pl.BlockSpec(memory_space=pl.ANY)
    dma = pltpu.SemaphoreType.DMA
    return pl.pallas_call(
        functools.partial(kernel, dims),
        out_shape=jax.ShapeDtypeStruct((rows, width), BF16),
        in_specs=[vmem, vmem, vmem, vmem, hbm, hbm, hbm, hbm, hbm, vmem],
        out_specs=vmem,
        scratch_shapes=[
            pltpu.VMEM((rows, width), BF16),
            pltpu.VMEM((n, CAP, width), BF16),
            pltpu.VMEM((n, CAP, width), BF16),
            pltpu.VMEM((n, CAP, width), BF16),
            pltpu.VMEM((n, CAP, width), BF16),
            pltpu.VMEM((width, ff), BF16),
            pltpu.VMEM((width, ff), BF16),
            pltpu.VMEM((ff, width), BF16),
            pltpu.VMEM((2,) + dims + (d_rows, dh), BF16),
            dma((5,)), dma((n,)), dma((n,)), dma((n,)), dma((n,)),
            dma((2, 4, n_z)), dma((2, 4, n_z)),
        ],
        compiler_params=pltpu.CompilerParams(
            collective_id=0, has_side_effects=True, vmem_limit_bytes=60 * 1024 * 1024
        ),
    )(
        tokens, norm_gain.reshape(1, -1), route_ids.T, route_weight.T,
        expert_gate, expert_up, expert_down, dense_up, dense_down.T, branch_gate.reshape(1, -1),
    )


def solution(mesh):
    placed = (
        P("ep", None), P(), P("ep", None), P("ep", None),
        P("ep", None, None), P("ep", None, None), P("ep", None, None),
        P("ep", None), P(None, "ep"), P(),
    )
    return jax.shard_map(
        on_device, mesh=mesh, in_specs=placed, out_specs=P("ep", None), check_vma=False
    )
```

```python
import functools
import math

import jax
import jax.numpy as jnp
from jax import lax
from jax.experimental import pallas as pl
from jax.experimental.pallas import tpu as pltpu
from jax.sharding import PartitionSpec as P

CAP = 8
F32 = jnp.float32
BF16 = jnp.bfloat16


def xor(a, b, size):
    out, bit = 0, 1
    while bit < size:
        out = out + ((a // bit) % 2 + (b // bit) % 2) % 2 * bit
        bit *= 2
    return out


def kernel(
    dims,
    tokens, gain, ids, weight, w_gate, w_up, w_down, d_up, d_down, branch,
    out,
    normed, send, recv, result, back, v_gate, v_up, v_down, wide,
    local_sem, out_send, out_recv, ret_send, ret_recv,
    w_send, w_recv,
):
    n_z, n_y, n_x, n_c = dims
    plane = n_y * n_x * n_c
    n = n_z * plane
    me = lax.axis_index("ep")
    my_z = me // plane
    my_in = me % plane
    my_c = me % n_c
    my_x = me // n_c % n_x
    my_y = me // (n_c * n_x) % n_y
    rows = tokens.shape[0]
    width = tokens.shape[1]
    experts = n
    slots = experts * CAP

    def dev(z, y, x, c):
        return ((z * n_y + y) * n_x + x) * n_c + c

    barrier = pltpu.get_barrier_semaphore()

    def greet(i, carry):
        pl.semaphore_signal(barrier, inc=1, device_id=((me + i) % n,), device_id_type=pl.DeviceIdType.MESH)
        return carry

    lax.fori_loop(1, n, greet, 0)

    own_up = pltpu.make_async_copy(d_up, wide.at[0, my_z, my_y, my_x, my_c], local_sem.at[0])
    own_down = pltpu.make_async_copy(d_down, wide.at[1, my_z, my_y, my_x, my_c], local_sem.at[1])
    own_up.start()
    own_down.start()
    loads = [
        pltpu.make_async_copy(w_gate.at[0], v_gate, local_sem.at[2]),
        pltpu.make_async_copy(w_up.at[0], v_up, local_sem.at[3]),
        pltpu.make_async_copy(w_down.at[0], v_down, local_sem.at[4]),
    ]
    for load in loads:
        load.start()

    x = tokens[...].astype(F32)
    scale = lax.rsqrt(jnp.mean(x * x, axis=-1, keepdims=True) + 1e-06)
    normed[...] = (x * scale * gain[...]).astype(BF16)

    id0, id1 = ids[0:1, :], ids[1:2, :]
    e_iota = lax.broadcasted_iota(jnp.int32, (experts, rows), 0)
    hot0 = (id0 == e_iota).astype(F32)
    hot1 = (id1 == e_iota).astype(F32)
    before = lax.broadcasted_iota(jnp.int32, (rows, rows), 0) < lax.broadcasted_iota(jnp.int32, (rows, rows), 1)
    count = jnp.dot((hot0 + hot1).astype(BF16), before.astype(F32).astype(BF16), preferred_element_type=F32)
    pos0 = id0 * CAP + jnp.sum(hot0 * count, axis=0, keepdims=True).astype(jnp.int32)
    pos1 = id1 * CAP + jnp.sum(hot1 * count, axis=0, keepdims=True).astype(jnp.int32)
    p_iota = lax.broadcasted_iota(jnp.int32, (slots, rows), 0)
    table0 = (pos0 == p_iota).astype(F32)
    table1 = (pos1 == p_iota).astype(F32)
    place = (table0 + table1).astype(BF16)
    packed = jnp.dot(place, normed[...], preferred_element_type=F32)
    send[...] = packed.reshape(n, CAP, width).astype(BF16)

    own_up.wait()
    own_down.wait()
    pl.semaphore_wait(barrier, n - 1)

    def remote(src, dst, s, r, target):
        return pltpu.make_async_remote_copy(
            src_ref=src, dst_ref=dst, send_sem=s, recv_sem=r,
            device_id=(target,), device_id_type=pl.DeviceIdType.MESH,
        )

    at = (my_z, my_y, my_x, my_c)
    orders = ((0, 1, 2, 3), (0, 2, 1, 3))

    def block_copy(half, stage, d, incoming):
        order = orders[half]
        axis = order[stage]
        origin = (at[axis] + dims[axis] - d) % dims[axis] if incoming else at[axis]
        where = [at[i] for i in range(4)]
        for held in order[:stage]:
            where[held] = slice(None)
        where[axis] = origin
        part = wide.at[(half,) + tuple(where)]
        target = [at[i] for i in range(4)]
        target[axis] = (at[axis] + d) % dims[axis]
        return remote(part, part, w_send.at[half, stage, d], w_recv.at[half, stage, d], dev(*target))

    def each(stage, act, incoming=False):
        for d in range(1, max(dims)):
            for half in range(2):
                if d < dims[orders[half][stage]]:
                    act(block_copy(half, stage, d, incoming))

    def begin(stage):
        each(stage, lambda copy: copy.start())

    def arrive(stage):
        each(stage, lambda copy: copy.wait_recv(), True)

    def leave(stage):
        each(stage, lambda copy: copy.wait_send())

    begin(0)

    def partner(step):
        z = xor(my_z, (step // plane + n_z // 2) % n_z, n_z)
        return z * plane + xor(my_in, step % plane, plane)

    own_step = (n_z - n_z // 2) * plane

    def over_others(first, last, body):
        def guarded(step, carry):
            body(partner(step))
            return carry

        if first <= own_step < last:
            lax.fori_loop(first, own_step, guarded, 0)
            lax.fori_loop(own_step + 1, last, guarded, 0)
        else:
            lax.fori_loop(first, last, guarded, 0)

    def dispatch(target, origin):
        return remote(send.at[target], recv.at[origin], out_send.at[target], out_recv.at[origin], target)

    def giveback(target, origin):
        return remote(result.at[target], back.at[origin], ret_send.at[target], ret_recv.at[origin], target)

    over_others(0, plane, lambda t: dispatch(t, me).start())
    arrive(0)
    begin(1)
    over_others(plane, n, lambda t: dispatch(t, me).start())
    recv[me] = send[me]

    for load in loads:
        load.wait()

    def experts_on(phase):
        z = xor(my_z, (phase + n_z // 2) % n_z, n_z)
        block = pl.ds(z * plane, plane)
        x_in = recv[block].reshape(plane * CAP, width)
        gate_part = jnp.dot(x_in, v_gate[...], preferred_element_type=F32)
        up_part = jnp.dot(x_in, v_up[...], preferred_element_type=F32)
        hidden = (gate_part / (1.0 + jnp.exp(-gate_part)) * up_part).astype(BF16)
        res = jnp.dot(hidden, v_down[...], preferred_element_type=F32)
        result[block] = res.reshape(plane, CAP, width).astype(BF16)

    def do_phase(phase):
        lo, hi = phase * plane, (phase + 1) * plane
        over_others(lo, hi, lambda t: dispatch(me, t).wait_recv())
        experts_on(phase)
        over_others(lo, hi, lambda t: giveback(t, me).start())

    for phase in range(n_z):
        do_phase(phase)
        if phase == 0:
            arrive(1)
            begin(2)
        if phase == 2:
            arrive(2)
            begin(3)
        if phase == 3:
            arrive(3)

    back[me] = result[me]

    dense_pre = jnp.dot(normed[...], wide[0].reshape(width, -1), preferred_element_type=F32)
    dense_hidden = (dense_pre / (1.0 + jnp.exp(-dense_pre))).astype(BF16)
    dense_out = lax.dot_general(
        dense_hidden, wide[1].reshape(width, -1), (((1,), (1,)), ((), ())), preferred_element_type=F32
    )
    dense_out = jnp.tanh(branch[...]) * dense_out

    share = table0 * weight[0:1, :] + table1 * weight[1:2, :]
    high = share.astype(BF16)
    low = (share - high.astype(F32)).astype(BF16)

    over_others(0, n, lambda t: giveback(me, t).wait_recv())
    rows_back = back[...].reshape(slots, width)
    across = (((0,), (0,)), ((), ()))
    combined = lax.dot_general(high, rows_back, across, preferred_element_type=F32)
    combined = combined + lax.dot_general(low, rows_back, across, preferred_element_type=F32)
    out[...] = (combined + dense_out).astype(BF16)

    over_others(0, n, lambda t: dispatch(t, me).wait_send())
    over_others(0, n, lambda t: giveback(t, me).wait_send())
    for stage in range(4):
        leave(stage)


def on_device(tokens, norm_gain, route_ids, route_weight, expert_gate, expert_up, expert_down, dense_up, dense_down, branch_gate):
    n = lax.axis_size("ep")
    assert expert_gate.shape[0] == 1
    rows, width = tokens.shape
    ff = expert_gate.shape[2]
    d_rows, dh = dense_up.shape
    n_z = 4
    side = math.isqrt(n // n_z // 2)
    dims = (n_z, side, side, 2)
    assert math.prod(dims) == n
    vmem = pl.BlockSpec(memory_space=pltpu.VMEM)
    hbm = pl.BlockSpec(memory_space=pl.ANY)
    dma = pltpu.SemaphoreType.DMA
    return pl.pallas_call(
        functools.partial(kernel, dims),
        out_shape=jax.ShapeDtypeStruct((rows, width), BF16),
        in_specs=[vmem, vmem, vmem, vmem, hbm, hbm, hbm, hbm, hbm, vmem],
        out_specs=vmem,
        scratch_shapes=[
            pltpu.VMEM((rows, width), BF16),
            pltpu.VMEM((n, CAP, width), BF16),
            pltpu.VMEM((n, CAP, width), BF16),
            pltpu.VMEM((n, CAP, width), BF16),
            pltpu.VMEM((n, CAP, width), BF16),
            pltpu.VMEM((width, ff), BF16),
            pltpu.VMEM((width, ff), BF16),
            pltpu.VMEM((ff, width), BF16),
            pltpu.VMEM((2,) + dims + (d_rows, dh), BF16),
            dma((5,)), dma((n,)), dma((n,)), dma((n,)), dma((n,)),
            dma((2, 4, n_z)), dma((2, 4, n_z)),
        ],
        compiler_params=pltpu.CompilerParams(
            collective_id=0, has_side_effects=True, vmem_limit_bytes=60 * 1024 * 1024
        ),
    )(
        tokens, norm_gain.reshape(1, -1), route_ids.T, route_weight.T,
        expert_gate, expert_up, expert_down, dense_up, dense_down.T, branch_gate.reshape(1, -1),
    )


def solution(mesh):
    placed = (
        P("ep", None), P(), P("ep", None), P("ep", None),
        P("ep", None, None), P("ep", None, None), P("ep", None, None),
        P("ep", None), P(None, "ep"), P(),
    )
    return jax.shard_map(
        on_device, mesh=mesh, in_specs=placed, out_specs=P("ep", None), check_vma=False
    )
```
